512 devices in a mesh: sp: 64 (over z, y), tp: 8 (over x, core).
Axes of the slice: x: 4, y: 4, z: 16, core: 2. Of those that a mesh axis runs over, the one named last changes fastest.
Arguments:
- stream_in: bfloat16 [16384, 2048], P('sp'), may hold values from -6 to 6
- norm_gain: float32 [2, 2048], replicated, may hold values from 0.1 to 1.9
- value_weight: bfloat16 [2, 2048, 2048], P(None, 'sp', 'tp'), may hold values from -0.125 to 0.125
- gate_weight: bfloat16 [2, 2048, 2048], P(None, 'sp', 'tp'), may hold values from -0.125 to 0.125
- conv_taps: float32 [2, 31, 2048], P(None, None, 'tp'), may hold values from -5 to 5
- channel_gain: float32 [2, 2048], P(None, 'tp'), may hold values from 0.1 to 1.9
- out_weight: bfloat16 [2, 2048, 2048], P(None, 'tp', 'sp'), may hold values from -0.125 to 0.125
Outputs:
- stream_out: bfloat16 [16384, 2048], P('sp')
The draws below stay inside these ranges and needn't reach their ends.
All inputs are finite; a program needn't handle non-finite values.
Results may differ from the reference program's by a relative error of at most 0.015.
Values may be sent and summed in bfloat16 or wider, within the bound.
No kernel may reach another device: no remote copies, remote signals or barrier semaphores. Data moves between devices by JAX's collectives and lax.ppermute only.
A program may use at most 64 MiB of HBM per device.

```python
import jax
import jax.numpy as jnp
from jax import lax

D = 2048
KERNEL = 31
LAYERS = 2
TOKENS = 16384


def draw_conv_taps(key, part):
    first, second = jax.random.split(jax.random.fold_in(key, 17))
    base = jnp.clip(jax.random.normal(first, (LAYERS, KERNEL, D), jnp.float32), -6.0, 6.0)
    blocks = jnp.exp(jax.random.uniform(second, (LAYERS, 1, 8), jnp.float32, -1.4, 1.4))
    scales = jnp.repeat(blocks, D // 8, axis=2)
    return base * scales / jnp.sqrt(jnp.float32(KERNEL))


def block_levels(key, shape, shards, low, top_value):
    def one(axis_at, parts):
        steps = jax.random.uniform(jax.random.fold_in(jax.random.fold_in(key, 6), axis_at), (parts,), jnp.float32, low / len(shards), top_value / len(shards))
        return jnp.repeat(jnp.exp(steps), shape[axis_at] // parts).reshape((-1,) + (1,) * (len(shape) - axis_at - 1))

    level = one(*shards[0])
    for cut in shards[1:]:
        level = level * one(*cut)
    return level


def scatter_about(rng, shape, width, limit, cuts=(), held_as=jnp.bfloat16):
    array = width * jax.random.normal(rng, shape, jnp.float32)
    if cuts:
        array = array * block_levels(rng, shape, cuts, -0.22, 0.18)
    return jnp.clip(array, -limit, limit).astype(held_as)


def setup_inputs(seed: int = 0) -> dict:
    splits = jax.random.split(jax.random.key(seed), 8)
    return {
        "stream_in": scatter_about(splits[0], (TOKENS, D), 1.0, 6.0, ((0, 64),)),
        "norm_gain": jnp.clip(1.0 + 0.18 * jax.random.normal(splits[1], (LAYERS, D), jnp.float32), 0.1, 1.9),
        "value_weight": scatter_about(splits[2], (LAYERS, D, D), D ** -0.5, 0.125, ((1, 64), (2, 8))),
        "gate_weight": scatter_about(splits[3], (LAYERS, D, D), D ** -0.5, 0.125, ((1, 64), (2, 8))),
        "conv_taps": draw_conv_taps(jax.random.fold_in(splits[7], 71), 0),
        "channel_gain": jnp.clip(1.0 + 0.18 * jax.random.normal(splits[5], (LAYERS, D), jnp.float32), 0.1, 1.9),
        "out_weight": scatter_about(splits[6], (LAYERS, D, D), D ** -0.5, 0.125, ((1, 8), (2, 64))),
    }


epsilon = 1e-05

def reference(stream_in, norm_gain, value_weight, gate_weight, conv_taps, channel_gain, out_weight):
    stream = stream_in
    for layer in range(LAYERS):
        wide = stream.astype(jnp.float32)
        normed = (wide * lax.rsqrt(lax.optimization_barrier(jnp.mean(wide * wide, axis=1, keepdims=True)) + epsilon) * norm_gain[layer]).astype(jnp.bfloat16)
        value = jnp.dot(normed, value_weight[layer], preferred_element_type=jnp.float32)
        gate = jnp.dot(normed, gate_weight[layer], preferred_element_type=jnp.float32)
        gated = (value * jax.nn.sigmoid(gate)).astype(jnp.bfloat16)
        padded = jnp.concatenate([jnp.zeros((KERNEL - 1, D), jnp.bfloat16), gated], axis=0).astype(jnp.float32)
        filtered = jnp.zeros((TOKENS, D), jnp.float32)
        for tap in range(KERNEL):
            filtered = filtered + conv_taps[layer, tap] * padded[tap:tap + TOKENS]
        mean_value = lax.optimization_barrier(jnp.mean(filtered, axis=1, keepdims=True))
        variance = lax.optimization_barrier(jnp.mean(filtered * filtered, axis=1, keepdims=True)) - mean_value * mean_value
        activated = jax.nn.silu((filtered - mean_value) * lax.rsqrt(variance + epsilon) * channel_gain[layer]).astype(jnp.bfloat16)
        branch = jnp.dot(activated, out_weight[layer], preferred_element_type=jnp.float32)
        stream = (wide + branch).astype(jnp.bfloat16)
    return stream
```

```python
import jax
import jax.numpy as jnp
from jax import lax
from jax.sharding import Mesh
from jax.sharding import PartitionSpec as P

LAYERS = 2
SP = ("z", "y")
TP = ("x", "c")
HALO = 32
epsilon = 1e-05


def shifted(value, axis, steps):
    count = lax.axis_size(axis)
    return lax.ppermute(value, axis, [(i, (i + steps) % count) for i in range(count)])


def passed_on(value, axes):
    count = lax.axis_size(axes)
    return lax.ppermute(value, axes, [(i, i + 1) for i in range(count - 1)])


def sent_to_all(shard, axis):
    copies = jnp.broadcast_to(shard, (lax.axis_size(axis), *shard.shape))
    return lax.all_to_all(copies, axis, split_axis=0, concat_axis=0, tiled=True)


def ring(block, axis):
    count = lax.axis_size(axis)
    ahead, behind = [], []
    up = down = block
    for step in range(1, count // 2 + 1):
        up = shifted(up, axis, 1)
        behind.append(up)
        if step < count - count // 2:
            down = shifted(down, axis, -1)
            ahead.append(down)
    return [block] + ahead + behind[::-1]


def body(stream_in, norm_gain, value_weight, gate_weight, conv_taps, channel_gain, out_weight):
    z, x, c = (lax.axis_index(a) for a in ("z", "x", "c"))
    width = stream_in.shape[1]
    half = stream_in.shape[0] // 2
    kernel = conv_taps.shape[1]
    cols = value_weight.shape[2]
    xs = lax.axis_size("x")
    share = half // xs

    before = passed_on(stream_in[-HALO:], SP)
    extended = jnp.concatenate([before, stream_in], axis=0)
    rows = lax.dynamic_slice_in_dim(extended, c * half, half + HALO, 0)

    raw = jnp.concatenate([value_weight, gate_weight, jnp.swapaxes(out_weight, 1, 2)], axis=2)
    near = sent_to_all(raw, "y")
    near = jnp.swapaxes(near, 0, 1).reshape(LAYERS, -1, raw.shape[2])
    pieces = ring(near, "z")

    small = jnp.concatenate([conv_taps, channel_gain[:, None]], axis=1)
    small = jnp.concatenate([small, shifted(small, "c", 1)], axis=2)

    stream = rows[HALO:]
    for layer in range(LAYERS):
        mine = jnp.concatenate([p[layer] for p in pieces], axis=0)
        other = shifted(mine, "c", 1)
        wide = rows.astype(jnp.float32)
        normed = (
            wide
            * lax.rsqrt(jnp.mean(wide * wide, axis=1, keepdims=True) + epsilon)
            * norm_gain[layer]
        ).astype(jnp.bfloat16)
        turned = lax.dynamic_slice_in_dim(
            jnp.concatenate([normed, normed], axis=1), z * (width // lax.axis_size("z")), width, 1
        )

        def product(at):
            return jnp.concatenate(
                [
                    jnp.dot(turned, w[:, at : at + cols], preferred_element_type=jnp.float32)
                    for w in (mine, other)
                ],
                axis=1,
            )

        gated = (product(0) * jax.nn.sigmoid(product(cols))).astype(jnp.bfloat16)
        if layer:
            tail = jnp.roll(gated[-HALO:], cols, axis=1)
            gated = jnp.concatenate([passed_on(tail, (*SP, "c")), gated], axis=0)
        padded = gated.astype(jnp.float32)
        taps = small[layer, :kernel]
        filtered = jnp.zeros((half, 2 * cols), jnp.float32)
        for tap in range(kernel):
            at = HALO - kernel + 1 + tap
            filtered = filtered + taps[tap] * padded[at : at + half]
        sums = jnp.stack([jnp.sum(filtered, axis=1), jnp.sum(filtered * filtered, axis=1)])
        sums = jnp.sum(sent_to_all(sums.reshape(1, -1), "x"), axis=0).reshape(2, half, 1)
        mean = sums[0] / width
        variance = sums[1] / width - mean * mean
        activated = jax.nn.silu(
            (filtered - mean) * lax.rsqrt(variance + epsilon) * small[layer, kernel]
        ).astype(jnp.bfloat16)
        out_t = jnp.concatenate([mine[:, 2 * cols :], other[:, 2 * cols :]], axis=1)
        branch = lax.dot_general(
            activated, out_t, (((1,), (1,)), ((), ())), preferred_element_type=jnp.float32
        ).astype(jnp.bfloat16)
        branch = lax.dynamic_slice_in_dim(
            jnp.concatenate([branch, branch], axis=1),
            width - z * (width // lax.axis_size("z")),
            width,
            1,
        )
        parts = lax.all_to_all(branch.reshape(xs, share, width), "x", 0, 0, tiled=True)
        own = lax.dynamic_slice_in_dim(stream, x * share, share, 0).astype(jnp.float32)
        own = (own + jnp.sum(parts.astype(jnp.float32), axis=0)).astype(jnp.bfloat16)
        stream = lax.all_gather(own, "x", axis=0, tiled=True)
        rows = stream
    sibling = shifted(stream, "c", 1)
    return jnp.where(
        c == 0,
        jnp.concatenate([stream, sibling], axis=0),
        jnp.concatenate([sibling, stream], axis=0),
    )


def solution(mesh):
    finer = Mesh(mesh.devices.reshape(16, 4, 4, 2), (*SP, *TP))
    placed = (
        P(SP, None),
        P(),
        P(None, SP, TP),
        P(None, SP, TP),
        P(None, None, TP),
        P(None, TP),
        P(None, TP, SP),
    )
    return jax.shard_map(body, mesh=finer, in_specs=placed, out_specs=P(SP, None), check_vma=False)
```

```python
import functools

import jax
import jax.numpy as jnp
from jax import lax
from jax.experimental import pallas as pl
from jax.experimental.pallas import tpu as pltpu
from jax.sharding import Mesh
from jax.sharding import PartitionSpec as P

SP = ("z", "y")
TP = ("x", "c")
HALO = 32
epsilon = 1e-05
F32 = jnp.float32
BF16 = jnp.bfloat16


def shifted(value, axis, steps):
    count = lax.axis_size(axis)
    return lax.ppermute(value, axis, [(i, (i + steps) % count) for i in range(count)])


def passed_on(value, axes):
    count = lax.axis_size(axes)
    return lax.ppermute(value, axes, [(i, i + 1) for i in range(count - 1)])


def sent_to_all(shard, axis):
    copies = jnp.broadcast_to(shard, (lax.axis_size(axis), *shard.shape))
    return lax.all_to_all(copies, axis, split_axis=0, concat_axis=0, tiled=True)


def in_parts(value):
    parts = []
    for _ in range(3):
        parts.append(lax.reduce_precision(value, 8, 7).astype(BF16))
        value = value - parts[-1].astype(F32)
    return jnp.stack(parts)


def call(kernel, out, *args, scratch=(), scalars=0):
    smem, vmem = pl.BlockSpec(memory_space=pltpu.SMEM), pl.BlockSpec(memory_space=pltpu.VMEM)
    return pl.pallas_call(
        kernel,
        out_shape=[jax.ShapeDtypeStruct(s, d) for s, d in out],
        in_specs=[smem] * scalars + [vmem] * (len(args) - scalars),
        out_specs=[vmem] * len(out),
        scratch_shapes=[pltpu.VMEM(s, d) for s, d in scratch],
    )(*args)


def normed(rows_ref, gain_ref, to_ref):
    count = rows_ref.shape[0]
    for at in range(0, count, HALO):
        wide = rows_ref[at : at + HALO, :].astype(F32)
        mean = jnp.mean(wide * wide, axis=1, keepdims=True)
        to_ref[at : at + HALO, :] = (wide * lax.rsqrt(mean + epsilon) * gain_ref[...]).astype(BF16)


def gate_of(a, w_ref, cols):
    value = jnp.dot(a, w_ref[:, :cols], preferred_element_type=F32)
    gate = jnp.dot(a, w_ref[:, cols : 2 * cols], preferred_element_type=F32)
    return (value * jax.nn.sigmoid(gate)).astype(BF16)


def first_kernel(cols, deep, ys, at_ref, rows_ref, gain_ref, small_ref, *refs):
    *blocks, pair_ref, keep_ref, send_ref, later_ref, last_ref, weights, scaled = refs
    later_ref[...] = pair_ref[:, : 2 * cols]
    last_ref[...] = pair_ref[:, 2 * cols : 3 * cols]
    here, c = at_ref[0], at_ref[1]
    whole = blocks[0].shape[0]
    for ref, offset, start in zip(blocks, (0, ys - 1, 1, 2, 2), (0, 0, 0, 0, whole // 2)):
        where = lax.rem(here + offset, ys) * deep
        for k in range(ref.shape[0] // deep):
            at = (start // deep + k) * ys * deep
            rows = pl.ds(pl.multiple_of(at + where, deep), deep)
            weights[rows, :] = ref[k * deep : (k + 1) * deep, : 2 * cols]
            send_ref[rows, :] = ref[k * deep : (k + 1) * deep, 2 * cols :]
    normed(rows_ref, gain_ref, scaled)
    gated = gate_of(scaled[...], weights, cols)
    count = keep_ref.shape[0]
    low, high = gated[:count], gated[rows_ref.shape[0] - count :]
    keep_ref[...] = jnp.where(c == 0, low, high)
    at = whole * ys
    send_ref[at : at + count, :] = jnp.where(c == 0, high, low)
    send_ref[at + count :, :] = small_ref[...]


def second_kernel(cols, rows_ref, gain_ref, mine_ref, other_ref, gated_ref, tail_ref, scaled):
    normed(rows_ref, gain_ref, scaled)
    for k, w_ref in enumerate((mine_ref, other_ref)):
        part = gate_of(scaled[...], w_ref, cols)
        gated_ref[:, k * cols : (k + 1) * cols] = part
        tail_ref[:, (1 - k) * cols : (2 - k) * cols] = part[-HALO:]


def meet_kernel(keep_ref, got_ref, padded_ref, other_ref):
    rows, cols = keep_ref.shape
    deep = other_ref.shape[0]
    at = got_ref.shape[0] - 3 * deep
    parts = [got_ref[at + k * deep : at + (k + 1) * deep, :].astype(F32) for k in range(3)]
    other_ref[...] = parts[0] + parts[1] + parts[2]
    padded_ref[:, :cols] = keep_ref[...].astype(F32)
    padded_ref[:, cols:] = got_ref[at - rows : at, :].astype(F32)


def body(stream_in, norm_gain, value_weight, gate_weight, conv_taps, channel_gain, out_weight):
    y, x, c = (lax.axis_index(a) for a in ("y", "x", "c"))
    width = stream_in.shape[1]
    half = stream_in.shape[0] // 2
    kernel = conv_taps.shape[1]
    cols = value_weight.shape[2]
    xs = lax.axis_size("x")
    share = half // xs

    raw = jnp.concatenate([value_weight, gate_weight, jnp.swapaxes(out_weight, 1, 2)], axis=2)
    deep, wide = raw.shape[1:]
    padded, first = lax.optimization_barrier((jnp.pad(raw[1], ((0, 0), (0, cols))), raw[0]))
    later = lax.all_gather(padded, "z", axis=0, tiled=True)
    block = lax.all_gather(first, "z", axis=0, tiled=True)
    block, edge = lax.optimization_barrier((block, stream_in[-HALO:]))
    before = passed_on(edge, SP)
    middle = block.shape[0] // 2
    up, down = shifted(block, "y", 1), shifted(block, "y", -1)
    blocks = (block, up, down, shifted(up[:middle], "y", 1), shifted(down[middle:], "y", -1))
    rows = jnp.concatenate([before, stream_in], axis=0)
    table = jnp.concatenate([conv_taps, channel_gain[:, None]], axis=1)
    small = in_parts(table).reshape(-1, cols)

    keep, send, later, last = call(
        functools.partial(first_kernel, cols, deep, lax.axis_size("y")),
        [
            ((half + HALO, cols), BF16),
            ((width + half + HALO + small.shape[0], cols), BF16),
            ((later.shape[0], 2 * cols), BF16),
            ((later.shape[0], cols), BF16),
        ],
        jnp.stack([y, c]),
        rows,
        norm_gain[:1],
        small,
        *blocks,
        later,
        scratch=[((width, 2 * cols), BF16), (rows.shape, BF16)],
        scalars=1,
    )
    later, last = (
        lax.all_gather(p.reshape(-1, 1, deep, p.shape[1]), "y", axis=1, tiled=True)
        for p in (later, last)
    )
    got = shifted(send, "c", 1)
    out_t = jnp.concatenate([send[:width], got[:width]], axis=1)
    padded, other_table = call(
        meet_kernel,
        [((half + HALO, 2 * cols), F32), ((2 * table.shape[1], cols), F32)],
        keep,
        got,
    )
    tables = jnp.concatenate([table, other_table.reshape(table.shape)], axis=2)

    stream = lax.dynamic_slice_in_dim(stream_in, c * half, half, 0)
    for layer in range(2):
        if layer:
            gated, tail = call(
                functools.partial(second_kernel, cols),
                [((half, 2 * cols), BF16), ((HALO, 2 * cols), BF16)],
                stream,
                norm_gain[1:],
                mine,
                other,
                scratch=[(stream.shape, BF16)],
            )
            padded = jnp.concatenate([passed_on(tail, (*SP, "c")), gated], axis=0).astype(F32)
        filtered = jnp.zeros((half, 2 * cols), F32)
        for tap in range(kernel):
            at = HALO - kernel + 1 + tap
            filtered = filtered + tables[layer, tap] * padded[at : at + half]
        sums = jnp.stack([jnp.sum(filtered, axis=1), jnp.sum(filtered * filtered, axis=1)])
        if layer:
            last, sums = lax.optimization_barrier((last, sums))
            last = last.reshape(width, cols)
            out_t = jnp.concatenate([last, shifted(last, "c", 1)], axis=1)
        sums = jnp.sum(lax.all_gather(sums.reshape(1, -1), "x", axis=0), axis=0).reshape(2, half, 1)
        mean = sums[0] / width
        variance = sums[1] / width - mean * mean
        gain = tables[layer, kernel]
        activated = jax.nn.silu((filtered - mean) * lax.rsqrt(variance + epsilon) * gain).astype(BF16)
        branch = lax.dot_general(
            activated, out_t, (((1,), (1,)), ((), ())), preferred_element_type=F32
        ).astype(BF16)
        parts = lax.all_to_all(branch.reshape(xs, share, width), "x", 0, 0, tiled=True)
        own = lax.dynamic_slice_in_dim(stream, x * share, share, 0).astype(F32)
        own = (own + jnp.sum(parts.astype(F32), axis=0)).astype(BF16)
        if not layer:
            later, own = lax.optimization_barrier((later, own))
            mine = later.reshape(width, 2 * cols)
            other = shifted(mine, "c", 1)
        stream = lax.all_gather(own, "x", axis=0, tiled=True)
    sibling = shifted(stream, "c", 1)
    return jnp.where(
        c == 0,
        jnp.concatenate([stream, sibling], axis=0),
        jnp.concatenate([sibling, stream], axis=0),
    )


def solution(mesh):
    finer = Mesh(mesh.devices.reshape(16, 4, 4, 2), (*SP, *TP))
    placed = (
        P(SP, None),
        P(),
        P(None, SP, TP),
        P(None, SP, TP),
        P(None, None, TP),
        P(None, TP),
        P(None, TP, SP),
    )
    return jax.shard_map(body, mesh=finer, in_specs=placed, out_specs=P(SP, None), check_vma=False)
```

```python
import functools

import jax
import jax.numpy as jnp
from jax import lax
from jax.experimental import pallas as pl
from jax.experimental.pallas import tpu as pltpu
from jax.sharding import Mesh
from jax.sharding import PartitionSpec as P

SP = ("z", "y")
TP = ("x", "c")
HALO = 32
epsilon = 1e-05
F32 = jnp.float32
BF16 = jnp.bfloat16


def shifted(value, axis, steps):
    count = lax.axis_size(axis)
    return lax.ppermute(value, axis, [(i, (i + steps) % count) for i in range(count)])


def passed_on(value, axes):
    count = lax.axis_size(axes)
    return lax.ppermute(value, axes, [(i, i + 1) for i in range(count - 1)])


def sent_to_all(shard, axis):
    copies = jnp.broadcast_to(shard, (lax.axis_size(axis), *shard.shape))
    return lax.all_to_all(copies, axis, split_axis=0, concat_axis=0, tiled=True)


def in_parts(value):
    parts = []
    for _ in range(3):
        parts.append(lax.reduce_precision(value, 8, 7).astype(BF16))
        value = value - parts[-1].astype(F32)
    return jnp.stack(parts)


def call(kernel, out, *args, scratch=(), scalars=0):
    smem, vmem = pl.BlockSpec(memory_space=pltpu.SMEM), pl.BlockSpec(memory_space=pltpu.VMEM)
    return pl.pallas_call(
        kernel,
        out_shape=[jax.ShapeDtypeStruct(s, d) for s, d in out],
        in_specs=[smem] * scalars + [vmem] * (len(args) - scalars),
        out_specs=[vmem] * len(out),
        scratch_shapes=[pltpu.VMEM(s, d) for s, d in scratch],
    )(*args)


def normed(rows_ref, gain_ref, to_ref):
    count = rows_ref.shape[0]
    for at in range(0, count, HALO):
        wide = rows_ref[at : at + HALO, :].astype(F32)
        mean = jnp.mean(wide * wide, axis=1, keepdims=True)
        to_ref[at : at + HALO, :] = (wide * lax.rsqrt(mean + epsilon) * gain_ref[...]).astype(BF16)


def gate_of(a, w_ref, cols):
    value = jnp.dot(a, w_ref[:, :cols], preferred_element_type=F32)
    gate = jnp.dot(a, w_ref[:, cols : 2 * cols], preferred_element_type=F32)
    return (value * jax.nn.sigmoid(gate)).astype(BF16)


def first_kernel(cols, deep, ys, at_ref, rows_ref, small_ref, *refs):
    *blocks, pair_ref, keep_ref, send_ref, later_ref, last_ref, weights = refs
    later_ref[...] = pair_ref[:, : 2 * cols]
    last_ref[...] = pair_ref[:, 2 * cols : 3 * cols]
    here, c = at_ref[0], at_ref[1]
    whole = blocks[0].shape[0]
    for ref, offset, start in zip(blocks, (0, ys - 1, 1, 2, 2), (0, 0, 0, 0, whole // 2)):
        where = lax.rem(here + offset, ys) * deep
        for k in range(ref.shape[0] // deep):
            at = (start // deep + k) * ys * deep
            rows = pl.ds(pl.multiple_of(at + where, deep), deep)
            weights[rows, :] = ref[k * deep : (k + 1) * deep, : 2 * cols]
            send_ref[rows, :] = ref[k * deep : (k + 1) * deep, 2 * cols :]
    gated = gate_of(rows_ref[...], weights, cols)
    count = keep_ref.shape[0]
    low, high = gated[:count], gated[rows_ref.shape[0] - count :]
    keep_ref[...] = jnp.where(c == 0, low, high)
    at = whole * ys
    send_ref[at : at + count, :] = jnp.where(c == 0, high, low)
    send_ref[at + count :, :] = small_ref[...]


def second_kernel(cols, rows_ref, gain_ref, later_ref, gated_ref, tail_ref, scaled, weights):
    normed(rows_ref, gain_ref, scaled)
    zs, cores, deep, _ = later_ref.shape
    for core in range(cores):
        for k in range(zs):
            weights[k * deep : (k + 1) * deep, :] = later_ref[k, core]
        part = gate_of(scaled[...], weights, cols)
        gated_ref[:, core * cols : (core + 1) * cols] = part
        tail_ref[:, core * cols : (core + 1) * cols] = part[-HALO:]


def meet_kernel(keep_ref, got_ref, padded_ref, other_ref):
    rows, cols = keep_ref.shape
    deep = other_ref.shape[0]
    at = got_ref.shape[0] - 3 * deep
    parts = [got_ref[at + k * deep : at + (k + 1) * deep, :].astype(F32) for k in range(3)]
    other_ref[...] = parts[0] + parts[1] + parts[2]
    padded_ref[:, :cols] = keep_ref[...].astype(F32)
    padded_ref[:, cols:] = got_ref[at - rows : at, :].astype(F32)


def body(stream_in, norm_gain, value_weight, gate_weight, conv_taps, channel_gain, out_weight):
    y, x, c = (lax.axis_index(a) for a in ("y", "x", "c"))
    width = stream_in.shape[1]
    half = stream_in.shape[0] // 2
    kernel = conv_taps.shape[1]
    cols = value_weight.shape[2]
    xs = lax.axis_size("x")
    share = half // xs

    turned = jnp.swapaxes(out_weight, 1, 2)
    first, padded = (
        jnp.concatenate([value_weight[k], gate_weight[k]] + [turned[k]] * (k + 1), axis=1)
        for k in range(2)
    )
    padded, first = lax.optimization_barrier((padded, first))
    deep = first.shape[0]
    later = lax.all_gather(padded, "z", axis=0, tiled=True)
    block = lax.all_gather(first, "z", axis=0, tiled=True)
    block, source = lax.optimization_barrier((block, stream_in))
    before = passed_on(source[-HALO:], SP)
    middle = block.shape[0] // 2
    up, down = shifted(block, "y", 1), shifted(block, "y", -1)
    up, down, before = lax.optimization_barrier((up, down, before))
    blocks = (block, up, down, shifted(up[:middle], "y", 1), shifted(down[middle:], "y", -1))
    rows = jnp.concatenate([before, stream_in], axis=0).astype(F32)
    rows = rows * lax.rsqrt(jnp.mean(rows * rows, axis=1, keepdims=True) + epsilon) * norm_gain[0]
    rows = rows.astype(BF16)
    table = jnp.concatenate([conv_taps, channel_gain[:, None]], axis=1)
    small = in_parts(table).reshape(-1, cols)

    keep, send, later, last = call(
        functools.partial(first_kernel, cols, deep, lax.axis_size("y")),
        [
            ((half + HALO, cols), BF16),
            ((width + half + HALO + small.shape[0], cols), BF16),
            ((later.shape[0], 2 * cols), BF16),
            ((later.shape[0], cols), BF16),
        ],
        jnp.stack([y, c]),
        rows,
        small,
        *blocks,
        later,
        scratch=[((width, 2 * cols), BF16)],
        scalars=1,
    )
    later, last = (
        lax.all_gather(p.reshape(-1, 1, deep, p.shape[1]), ("c", "y"), axis=1, tiled=True)
        for p in (later, last)
    )
    got = shifted(send, "c", 1)
    out_t = jnp.concatenate([send[:width], got[:width]], axis=1)
    padded, other_table = call(
        meet_kernel,
        [((half + HALO, 2 * cols), F32), ((2 * table.shape[1], cols), F32)],
        keep,
        got,
    )
    pair = (table, other_table.reshape(table.shape))
    ordered = jnp.where(c == 0, jnp.concatenate(pair, 2)[1], jnp.concatenate(pair[::-1], 2)[1])
    tables = (jnp.concatenate(pair, 2)[0], ordered)

    stream = lax.dynamic_slice_in_dim(stream_in, c * half, half, 0)
    for layer in range(2):
        if layer:
            gated, tail = call(
                functools.partial(second_kernel, cols),
                [((half, 2 * cols), BF16), ((HALO, 2 * cols), BF16)],
                stream,
                norm_gain[1:],
                later.reshape(lax.axis_size("z"), 2, -1, 2 * cols),
                scratch=[(stream.shape, BF16), ((width, 2 * cols), BF16)],
            )
            padded = jnp.concatenate([passed_on(tail, (*SP, "c")), gated], axis=0).astype(F32)
        filtered = jnp.zeros((half, 2 * cols), F32)
        for tap in range(kernel):
            at = HALO - kernel + 1 + tap
            filtered = filtered + tables[layer][tap] * padded[at : at + half]
        sums = jnp.stack([jnp.sum(filtered, axis=1), jnp.sum(filtered * filtered, axis=1)])
        sums = jnp.sum(lax.all_gather(sums.reshape(1, -1), "x", axis=0), axis=0).reshape(2, half, 1)
        if layer:
            last, sums = lax.optimization_barrier((last, sums))
            last = last.reshape(lax.axis_size("z"), 2, -1, cols)
            out_t = jnp.concatenate([last[:, k].reshape(width, cols) for k in range(2)], axis=1)
        mean = sums[0] / width
        variance = sums[1] / width - mean * mean
        gain = tables[layer][kernel]
        activated = jax.nn.silu((filtered - mean) * lax.rsqrt(variance + epsilon) * gain).astype(BF16)
        branch = lax.dot_general(
            activated, out_t, (((1,), (1,)), ((), ())), preferred_element_type=F32
        ).astype(BF16)
        parts = lax.all_to_all(branch.reshape(xs, share, width), "x", 0, 0, tiled=True)
        own = lax.dynamic_slice_in_dim(stream, x * share, share, 0).astype(F32)
        own = (own + jnp.sum(parts.astype(F32), axis=0)).astype(BF16)
        stream = lax.all_gather(own, "x", axis=0, tiled=True)
    sibling = shifted(stream, "c", 1)
    return jnp.where(
        c == 0,
        jnp.concatenate([stream, sibling], axis=0),
        jnp.concatenate([sibling, stream], axis=0),
    )


def solution(mesh):
    finer = Mesh(mesh.devices.reshape(16, 4, 4, 2), (*SP, *TP))
    placed = (
        P(SP, None),
        P(),
        P(None, SP, TP),
        P(None, SP, TP),
        P(None, None, TP),
        P(None, TP),
        P(None, TP, SP),
    )
    return jax.shard_map(body, mesh=finer, in_specs=placed, out_specs=P(SP, None), check_vma=False)
```

```python
import functools

import jax
import jax.numpy as jnp
from jax import lax
from jax.experimental import pallas as pl
from jax.experimental.pallas import tpu as pltpu
from jax.sharding import Mesh
from jax.sharding import PartitionSpec as P

SP = ("z", "y")
TP = ("x", "c")
HALO = 32
epsilon = 1e-05
F32 = jnp.float32
BF16 = jnp.bfloat16


def shifted(value, axis, steps):
    count = lax.axis_size(axis)
    return lax.ppermute(value, axis, [(i, (i + steps) % count) for i in range(count)])


def passed_on(value, axes):
    count = lax.axis_size(axes)
    return lax.ppermute(value, axes, [(i, i + 1) for i in range(count - 1)])


def sent_to_all(shard, axis):
    copies = jnp.broadcast_to(shard, (lax.axis_size(axis), *shard.shape))
    return lax.all_to_all(copies, axis, split_axis=0, concat_axis=0, tiled=True)


def in_parts(value):
    parts = []
    for _ in range(3):
        parts.append(lax.reduce_precision(value, 8, 7).astype(BF16))
        value = value - parts[-1].astype(F32)
    return jnp.stack(parts)


def call(kernel, out, *args, scratch=(), scalars=0, last=None):
    smem, vmem = pl.BlockSpec(memory_space=pltpu.SMEM), pl.BlockSpec(memory_space=pltpu.VMEM)
    return pl.pallas_call(
        kernel,
        out_shape=[jax.ShapeDtypeStruct(s, d) for s, d in out],
        grid=(1,) if last else (),
        in_specs=[smem] * scalars + [vmem] * (len(args) - scalars - 1) + [last or vmem],
        out_specs=[vmem] * len(out),
        scratch_shapes=[pltpu.VMEM(s, d) for s, d in scratch],
    )(*args)


def normed(rows_ref, gain_ref, to_ref):
    count = rows_ref.shape[0]
    for at in range(0, count, HALO):
        wide = rows_ref[at : at + HALO, :].astype(F32)
        mean = jnp.mean(wide * wide, axis=1, keepdims=True)
        to_ref[at : at + HALO, :] = (wide * lax.rsqrt(mean + epsilon) * gain_ref[...]).astype(BF16)


def gate_of(a, w_ref, cols):
    value = jnp.dot(a, w_ref[:, :cols], preferred_element_type=F32)
    gate = jnp.dot(a, w_ref[:, cols : 2 * cols], preferred_element_type=F32)
    return (value * jax.nn.sigmoid(gate)).astype(BF16)


def first_kernel(cols, deep, ys, at_ref, rows_ref, small_ref, *refs):
    *blocks, pair_ref, keep_ref, send_ref, later_ref, weights = refs
    later_ref[...] = pair_ref[:, : 3 * cols]
    here, c = at_ref[0], at_ref[1]
    whole = blocks[0].shape[0]
    for ref, offset, start in zip(blocks, (0, ys - 1, 1, 2, 2), (0, 0, 0, 0, whole // 2)):
        where = lax.rem(here + offset, ys) * deep
        for k in range(ref.shape[0] // deep):
            at = (start // deep + k) * ys * deep
            rows = pl.ds(pl.multiple_of(at + where, deep), deep)
            weights[rows, :] = ref[k * deep : (k + 1) * deep, : 2 * cols]
            send_ref[rows, :] = ref[k * deep : (k + 1) * deep, 2 * cols :]
    gated = gate_of(rows_ref[...], weights, cols)
    count = keep_ref.shape[0]
    low, high = gated[:count], gated[rows_ref.shape[0] - count :]
    keep_ref[...] = jnp.where(c == 0, low, high)
    at = whole * ys
    send_ref[at : at + count, :] = jnp.where(c == 0, high, low)
    send_ref[at + count :, :] = small_ref[...]


def second_kernel(cols, rows_ref, gain_ref, later_ref, gated_ref, tail_ref, scaled, weights):
    normed(rows_ref, gain_ref, scaled)
    zs, cores, deep, _ = later_ref.shape
    for core in range(cores):
        for k in range(zs):
            weights[k * deep : (k + 1) * deep, :] = later_ref[k, core]
        part = gate_of(scaled[...], weights, cols)
        gated_ref[:, core * cols : (core + 1) * cols] = part
        tail_ref[:, core * cols : (core + 1) * cols] = part[-HALO:]


def meet_kernel(keep_ref, got_ref, padded_ref, other_ref):
    rows, cols = keep_ref.shape
    deep = other_ref.shape[0]
    at = got_ref.shape[0] - 3 * deep
    parts = [got_ref[at + k * deep : at + (k + 1) * deep, :].astype(F32) for k in range(3)]
    other_ref[...] = parts[0] + parts[1] + parts[2]
    padded_ref[:, :cols] = keep_ref[...].astype(F32)
    padded_ref[:, cols:] = got_ref[at - rows : at, :].astype(F32)


def body(stream_in, norm_gain, value_weight, gate_weight, conv_taps, channel_gain, out_weight):
    y, x, c = (lax.axis_index(a) for a in ("y", "x", "c"))
    width = stream_in.shape[1]
    half = stream_in.shape[0] // 2
    kernel = conv_taps.shape[1]
    cols = value_weight.shape[2]
    xs = lax.axis_size("x")
    share = half // xs

    turned = jnp.swapaxes(out_weight, 1, 2)
    first, padded = (
        jnp.concatenate([value_weight[k], gate_weight[k]] + [turned[k]] * (k + 1), axis=1)
        for k in range(2)
    )
    padded, first = lax.optimization_barrier((padded, first))
    deep = first.shape[0]
    later = lax.all_gather(padded, "z", axis=0, tiled=True)
    block = lax.all_gather(first, "z", axis=0, tiled=True)
    block, source = lax.optimization_barrier((block, stream_in))
    before = passed_on(source[-HALO:], SP)
    middle = block.shape[0] // 2
    up, down = shifted(block, "y", 1), shifted(block, "y", -1)
    up, down, before = lax.optimization_barrier((up, down, before))
    blocks = (block, up, down, shifted(up[:middle], "y", 1), shifted(down[middle:], "y", -1))
    rows = jnp.concatenate([before, stream_in], axis=0).astype(F32)
    rows = rows * lax.rsqrt(jnp.mean(rows * rows, axis=1, keepdims=True) + epsilon) * norm_gain[0]
    rows = rows.astype(BF16)
    table = jnp.concatenate([conv_taps, channel_gain[:, None]], axis=1)
    small = in_parts(table).reshape(-1, cols)

    keep, send, later = call(
        functools.partial(first_kernel, cols, deep, lax.axis_size("y")),
        [
            ((half + HALO, cols), BF16),
            ((width + half + HALO + small.shape[0], cols), BF16),
            ((later.shape[0], 3 * cols), BF16),
        ],
        jnp.stack([y, c]),
        rows,
        small,
        *blocks,
        later,
        scratch=[((width, 2 * cols), BF16)],
        scalars=1,
    )
    later = lax.all_gather(
        later.reshape(-1, 1, deep, later.shape[1]), ("c", "y"), axis=1, tiled=True
    ).reshape(lax.axis_size("z"), 2, -1, later.shape[1])
    got = shifted(send, "c", 1)
    out_t = jnp.concatenate([send[:width], got[:width]], axis=1)
    padded, other_table = call(
        meet_kernel,
        [((half + HALO, 2 * cols), F32), ((2 * table.shape[1], cols), F32)],
        keep,
        got,
    )
    pair = (table, other_table.reshape(table.shape))
    ordered = jnp.where(c == 0, jnp.concatenate(pair, 2)[1], jnp.concatenate(pair[::-1], 2)[1])
    tables = (jnp.concatenate(pair, 2)[0], ordered)

    stream = lax.dynamic_slice_in_dim(stream_in, c * half, half, 0)
    for layer in range(2):
        if layer:
            gated, tail = call(
                functools.partial(second_kernel, cols),
                [((half, 2 * cols), BF16), ((HALO, 2 * cols), BF16)],
                stream,
                norm_gain[1:],
                later,
                scratch=[(stream.shape, BF16), ((width, 2 * cols), BF16)],
                last=pl.BlockSpec((*later.shape[:3], 2 * cols), lambda _: (0, 0, 0, 0)),
            )
            columns, tail = lax.optimization_barrier((later, tail))
            columns = columns[..., 2 * cols :]
            out_t = jnp.concatenate([columns[:, k].reshape(width, cols) for k in range(2)], axis=1)
            padded = jnp.concatenate([passed_on(tail, (*SP, "c")), gated], axis=0).astype(F32)
        filtered = jnp.zeros((half, 2 * cols), F32)
        for tap in range(kernel):
            at = HALO - kernel + 1 + tap
            filtered = filtered + tables[layer][tap] * padded[at : at + half]
        sums = jnp.stack([jnp.sum(filtered, axis=1), jnp.sum(filtered * filtered, axis=1)])
        sums = jnp.sum(lax.all_gather(sums.reshape(1, -1), "x", axis=0), axis=0).reshape(2, half, 1)
        mean = sums[0] / width
        variance = sums[1] / width - mean * mean
        gain = tables[layer][kernel]
        activated = jax.nn.silu((filtered - mean) * lax.rsqrt(variance + epsilon) * gain).astype(BF16)
        branch = lax.dot_general(
            activated, out_t, (((1,), (1,)), ((), ())), preferred_element_type=F32
        ).astype(BF16)
        parts = lax.all_to_all(branch.reshape(xs, share, width), "x", 0, 0, tiled=True)
        own = lax.dynamic_slice_in_dim(stream, x * share, share, 0).astype(F32)
        own = (own + jnp.sum(parts.astype(F32), axis=0)).astype(BF16)
        stream = lax.all_gather(own, "x", axis=0, tiled=True)
    sibling = shifted(stream, "c", 1)
    return jnp.where(
        c == 0,
        jnp.concatenate([stream, sibling], axis=0),
        jnp.concatenate([sibling, stream], axis=0),
    )


def solution(mesh):
    finer = Mesh(mesh.devices.reshape(16, 4, 4, 2), (*SP, *TP))
    placed = (
        P(SP, None),
        P(),
        P(None, SP, TP),
        P(None, SP, TP),
        P(None, None, TP),
        P(None, TP),
        P(None, TP, SP),
    )
    return jax.shard_map(body, mesh=finer, in_specs=placed, out_specs=P(SP, None), check_vma=False)
```

```python
import functools

import jax
import jax.numpy as jnp
from jax import lax
from jax.experimental import pallas as pl
from jax.experimental.pallas import tpu as pltpu
from jax.sharding import Mesh
from jax.sharding import PartitionSpec as P

SP = ("z", "y")
TP = ("x", "c")
HALO = 32
epsilon = 1e-05
F32 = jnp.float32
BF16 = jnp.bfloat16


def shifted(value, axis, steps):
    count = lax.axis_size(axis)
    return lax.ppermute(value, axis, [(i, (i + steps) % count) for i in range(count)])


def passed_on(value, axes):
    count = lax.axis_size(axes)
    return lax.ppermute(value, axes, [(i, i + 1) for i in range(count - 1)])


def sent_to_all(shard, axis):
    copies = jnp.broadcast_to(shard, (lax.axis_size(axis), *shard.shape))
    return lax.all_to_all(copies, axis, split_axis=0, concat_axis=0, tiled=True)


def in_parts(value):
    parts = []
    for _ in range(3):
        parts.append(lax.reduce_precision(value, 8, 7).astype(BF16))
        value = value - parts[-1].astype(F32)
    return jnp.stack(parts)


def call(kernel, out, *args, scratch=(), scalars=0, last=None):
    smem, vmem = pl.BlockSpec(memory_space=pltpu.SMEM), pl.BlockSpec(memory_space=pltpu.VMEM)
    return pl.pallas_call(
        kernel,
        out_shape=[jax.ShapeDtypeStruct(s, d) for s, d in out],
        grid=(1,) if last else (),
        in_specs=[smem] * scalars + [vmem] * (len(args) - scalars - 1) + [last or vmem],
        out_specs=[vmem] * len(out),
        scratch_shapes=[pltpu.VMEM(s, d) for s, d in scratch],
    )(*args)


def normed(rows_ref, gain_ref, to_ref):
    count = rows_ref.shape[0]
    for at in range(0, count, HALO):
        wide = rows_ref[at : at + HALO, :].astype(F32)
        mean = jnp.mean(wide * wide, axis=1, keepdims=True)
        to_ref[at : at + HALO, :] = (wide * lax.rsqrt(mean + epsilon) * gain_ref[...]).astype(BF16)


def gate_of(a, w_ref, cols):
    value = jnp.dot(a, w_ref[:, :cols], preferred_element_type=F32)
    gate = jnp.dot(a, w_ref[:, cols : 2 * cols], preferred_element_type=F32)
    return (value * jax.nn.sigmoid(gate)).astype(BF16)


def first_kernel(cols, deep, ys, at_ref, rows_ref, small_ref, *refs):
    *blocks, pair_ref, keep_ref, send_ref, later_ref, weights = refs
    later_ref[...] = pair_ref[:, : 3 * cols]
    here, c = at_ref[0], at_ref[1]
    whole = blocks[0].shape[0]
    for ref, offset, start in zip(blocks, (0, ys - 1, 1, 2, 2), (0, 0, 0, 0, whole // 2)):
        where = lax.rem(here + offset, ys) * deep
        for k in range(ref.shape[0] // deep):
            at = (start // deep + k) * ys * deep
            rows = pl.ds(pl.multiple_of(at + where, deep), deep)
            weights[rows, :] = ref[k * deep : (k + 1) * deep, : 2 * cols]
            send_ref[rows, :] = ref[k * deep : (k + 1) * deep, 2 * cols :]
    gated = gate_of(rows_ref[...], weights, cols)
    count = keep_ref.shape[0]
    low, high = gated[:count], gated[rows_ref.shape[0] - count :]
    keep_ref[...] = jnp.where(c == 0, low, high)
    at = whole * ys
    send_ref[at : at + count, :] = jnp.where(c == 0, high, low)
    send_ref[at + count :, :] = small_ref[...]


def second_kernel(cols, rows_ref, gain_ref, later_ref, gated_ref, tail_ref, scaled, weights):
    normed(rows_ref, gain_ref, scaled)
    zs, cores, deep, _ = later_ref.shape
    for core in range(cores):
        for k in range(zs):
            weights[k * deep : (k + 1) * deep, :] = later_ref[k, core]
        part = gate_of(scaled[...], weights, cols)
        gated_ref[:, core * cols : (core + 1) * cols] = part
        tail_ref[:, core * cols : (core + 1) * cols] = part[-HALO:]


def meet_kernel(keep_ref, got_ref, padded_ref, other_ref):
    rows, cols = keep_ref.shape
    deep = other_ref.shape[0]
    at = got_ref.shape[0] - 3 * deep
    parts = [got_ref[at + k * deep : at + (k + 1) * deep, :].astype(F32) for k in range(3)]
    other_ref[...] = parts[0] + parts[1] + parts[2]
    padded_ref[:, :cols] = keep_ref[...].astype(F32)
    padded_ref[:, cols:] = got_ref[at - rows : at, :].astype(F32)


def body(stream_in, norm_gain, value_weight, gate_weight, conv_taps, channel_gain, out_weight):
    y, x, c = (lax.axis_index(a) for a in ("y", "x", "c"))
    width = stream_in.shape[1]
    half = stream_in.shape[0] // 2
    kernel = conv_taps.shape[1]
    cols = value_weight.shape[2]
    xs = lax.axis_size("x")
    share = half // xs

    turned = jnp.swapaxes(out_weight, 1, 2)
    first, padded = (
        jnp.concatenate([value_weight[k], gate_weight[k]] + [turned[k]] * (k + 1), axis=1)
        for k in range(2)
    )
    padded, first = lax.optimization_barrier((padded, first))
    deep = first.shape[0]
    later = lax.all_gather(padded, "z", axis=0, tiled=True)
    block = lax.all_gather(first, "z", axis=0, tiled=True)
    block, source = lax.optimization_barrier((block, stream_in))
    before = passed_on(source[-HALO:], SP)
    middle = block.shape[0] // 2
    up, down = shifted(block, "y", 1), shifted(block, "y", -1)
    up, down, before = lax.optimization_barrier((up, down, before))
    blocks = (block, up, down, shifted(up[:middle], "y", 1), shifted(down[middle:], "y", -1))
    rows = jnp.concatenate([before, stream_in], axis=0).astype(F32)
    rows = rows * lax.rsqrt(jnp.mean(rows * rows, axis=1, keepdims=True) + epsilon) * norm_gain[0]
    rows = rows.astype(BF16)
    table = jnp.concatenate([conv_taps, channel_gain[:, None]], axis=1)
    small = in_parts(table).reshape(-1, cols)

    keep, send, later = call(
        functools.partial(first_kernel, cols, deep, lax.axis_size("y")),
        [
            ((half + HALO, cols), BF16),
            ((width + half + HALO + small.shape[0], cols), BF16),
            ((later.shape[0], 3 * cols), BF16),
        ],
        jnp.stack([y, c]),
        rows,
        small,
        *blocks,
        later,
        scratch=[((width, 2 * cols), BF16)],
        scalars=1,
    )
    later = lax.all_gather(
        later.reshape(-1, 1, deep, later.shape[1]), ("c", "y"), axis=1, tiled=True
    ).reshape(lax.axis_size("z"), 2, -1, later.shape[1])
    got = shifted(send, "c", 1)
    out_t = jnp.concatenate([send[:width], got[:width]], axis=1)
    padded, other_table = call(
        meet_kernel,
        [((half + HALO, 2 * cols), F32), ((2 * table.shape[1], cols), F32)],
        keep,
        got,
    )
    pair = (table, other_table.reshape(table.shape))
    ordered = jnp.where(c == 0, jnp.concatenate(pair, 2)[1], jnp.concatenate(pair[::-1], 2)[1])
    tables = (jnp.concatenate(pair, 2)[0], ordered)

    stream = lax.dynamic_slice_in_dim(stream_in, c * half, half, 0)
    for layer in range(2):
        if layer:
            gated, tail = call(
                functools.partial(second_kernel, cols),
                [((half, 2 * cols), BF16), ((HALO, 2 * cols), BF16)],
                stream,
                norm_gain[1:],
                later,
                scratch=[(stream.shape, BF16), ((width, 2 * cols), BF16)],
                last=pl.BlockSpec((*later.shape[:3], 2 * cols), lambda _: (0, 0, 0, 0)),
            )
            columns, tail = lax.optimization_barrier((later, tail))
            columns = columns[..., 2 * cols :]
            out_t = jnp.concatenate([columns[:, k].reshape(width, cols) for k in range(2)], axis=1)
            padded = jnp.concatenate([passed_on(tail, (*SP, "c")), gated], axis=0).astype(F32)
        filtered = jnp.zeros((half, 2 * cols), F32)
        for tap in range(kernel):
            at = HALO - kernel + 1 + tap
            filtered = filtered + tables[layer][tap] * padded[at : at + half]
        sums = jnp.stack([jnp.sum(filtered, axis=1), jnp.sum(filtered * filtered, axis=1)])
        sums = jnp.sum(lax.all_gather(sums.reshape(1, -1), "x", axis=0), axis=0).reshape(2, half, 1)
        mean = sums[0] / width
        variance = sums[1] / width - mean * mean
        gain = tables[layer][kernel]
        activated = jax.nn.silu((filtered - mean) * lax.rsqrt(variance + epsilon) * gain).astype(BF16)
        branch = lax.dot_general(
            activated, out_t, (((1,), (1,)), ((), ())), preferred_element_type=F32
        ).astype(BF16)
        parts = lax.all_to_all(branch.reshape(xs, share, width), "x", 0, 0, tiled=True)
        own = lax.dynamic_slice_in_dim(stream, x * share, share, 0).astype(F32)
        own = (own + jnp.sum(parts.astype(F32), axis=0)).astype(BF16)
        stream = sent_to_all(own, "x").reshape(half, width)
    sibling = shifted(stream, "c", 1)
    return jnp.where(
        c == 0,
        jnp.concatenate([stream, sibling], axis=0),
        jnp.concatenate([sibling, stream], axis=0),
    )


def solution(mesh):
    finer = Mesh(mesh.devices.reshape(16, 4, 4, 2), (*SP, *TP))
    placed = (
        P(SP, None),
        P(),
        P(None, SP, TP),
        P(None, SP, TP),
        P(None, None, TP),
        P(None, TP),
        P(None, TP, SP),
    )
    return jax.shard_map(body, mesh=finer, in_specs=placed, out_specs=P(SP, None), check_vma=False)
```

```python
import functools

import jax
import jax.numpy as jnp
from jax import lax
from jax.experimental import pallas as pl
from jax.experimental.pallas import tpu as pltpu
from jax.sharding import Mesh
from jax.sharding import PartitionSpec as P

SP = ("z", "y")
TP = ("x", "c")
HALO = 32
epsilon = 1e-05
F32 = jnp.float32
BF16 = jnp.bfloat16


def shifted(value, axis, steps):
    count = lax.axis_size(axis)
    return lax.ppermute(value, axis, [(i, (i + steps) % count) for i in range(count)])


def passed_on(value, axes):
    count = lax.axis_size(axes)
    return lax.ppermute(value, axes, [(i, i + 1) for i in range(count - 1)])


def sent_to_all(shard, axis):
    copies = jnp.broadcast_to(shard, (lax.axis_size(axis), *shard.shape))
    return lax.all_to_all(copies, axis, split_axis=0, concat_axis=0, tiled=True)


def in_parts(value):
    parts = []
    for _ in range(3):
        parts.append(lax.reduce_precision(value, 8, 7).astype(BF16))
        value = value - parts[-1].astype(F32)
    return jnp.stack(parts)


def call(kernel, out, *args, scratch=(), scalars=0, last=None):
    smem, vmem = pl.BlockSpec(memory_space=pltpu.SMEM), pl.BlockSpec(memory_space=pltpu.VMEM)
    return pl.pallas_call(
        kernel,
        out_shape=[jax.ShapeDtypeStruct(s, d) for s, d in out],
        grid=(1,) if last else (),
        in_specs=[smem] * scalars + [vmem] * (len(args) - scalars - 1) + [last or vmem],
        out_specs=[vmem] * len(out),
        scratch_shapes=[pltpu.VMEM(s, d) for s, d in scratch],
    )(*args)


def normed(rows_ref, gain_ref, to_ref):
    count = rows_ref.shape[0]
    for at in range(0, count, HALO):
        wide = rows_ref[at : at + HALO, :].astype(F32)
        mean = jnp.mean(wide * wide, axis=1, keepdims=True)
        to_ref[at : at + HALO, :] = (wide * lax.rsqrt(mean + epsilon) * gain_ref[...]).astype(BF16)


def gate_of(a, w_ref, cols):
    value = jnp.dot(a, w_ref[:, :cols], preferred_element_type=F32)
    gate = jnp.dot(a, w_ref[:, cols : 2 * cols], preferred_element_type=F32)
    return (value * jax.nn.sigmoid(gate)).astype(BF16)


def first_kernel(cols, deep, ys, at_ref, rows_ref, small_ref, *refs):
    *blocks, pair_ref, keep_ref, send_ref, later_ref, weights = refs
    later_ref[...] = pair_ref[:, : 3 * cols]
    here, c = at_ref[0], at_ref[1]
    whole = blocks[0].shape[0]
    for ref, offset, start in zip(blocks, (0, ys - 1, 1, 2, 2), (0, 0, 0, 0, whole // 2)):
        where = lax.rem(here + offset, ys) * deep
        for k in range(ref.shape[0] // deep):
            at = (start // deep + k) * ys * deep
            rows = pl.ds(pl.multiple_of(at + where, deep), deep)
            weights[rows, :] = ref[k * deep : (k + 1) * deep, : 2 * cols]
            send_ref[rows, :] = ref[k * deep : (k + 1) * deep, 2 * cols :]
    gated = gate_of(rows_ref[...], weights, cols)
    count = keep_ref.shape[0]
    low, high = gated[:count], gated[rows_ref.shape[0] - count :]
    keep_ref[...] = jnp.where(c == 0, low, high)
    at = whole * ys
    send_ref[at : at + count, :] = jnp.where(c == 0, high, low)
    send_ref[at + count :, :] = small_ref[...]


def second_kernel(cols, rows_ref, gain_ref, later_ref, gated_ref, tail_ref, scaled):
    normed(rows_ref, gain_ref, scaled)
    zs, cores, deep, wide = later_ref.shape
    for core in range(cores):
        part = gate_of(scaled[...], later_ref[:, core].reshape(zs * deep, wide), cols)
        gated_ref[:, core * cols : (core + 1) * cols] = part
        tail_ref[:, core * cols : (core + 1) * cols] = part[-HALO:]


def meet_kernel(keep_ref, got_ref, padded_ref, other_ref):
    rows, cols = keep_ref.shape
    deep = other_ref.shape[0]
    at = got_ref.shape[0] - 3 * deep
    parts = [got_ref[at + k * deep : at + (k + 1) * deep, :].astype(F32) for k in range(3)]
    other_ref[...] = parts[0] + parts[1] + parts[2]
    padded_ref[:, :cols] = keep_ref[...].astype(F32)
    padded_ref[:, cols:] = got_ref[at - rows : at, :].astype(F32)


def body(stream_in, norm_gain, value_weight, gate_weight, conv_taps, channel_gain, out_weight):
    y, x, c = (lax.axis_index(a) for a in ("y", "x", "c"))
    width = stream_in.shape[1]
    half = stream_in.shape[0] // 2
    kernel = conv_taps.shape[1]
    cols = value_weight.shape[2]
    xs = lax.axis_size("x")
    share = half // xs

    turned = jnp.swapaxes(out_weight, 1, 2)
    first, padded = (
        jnp.concatenate([value_weight[k], gate_weight[k]] + [turned[k]] * (k + 1), axis=1)
        for k in range(2)
    )
    padded, first = lax.optimization_barrier((padded, first))
    deep = first.shape[0]
    later = lax.all_gather(padded, "z", axis=0, tiled=True)
    block = lax.all_gather(first, "z", axis=0, tiled=True)
    block, source = lax.optimization_barrier((block, stream_in))
    before = passed_on(source[-HALO:], SP)
    middle = block.shape[0] // 2
    up, down = shifted(block, "y", 1), shifted(block, "y", -1)
    up, down, before = lax.optimization_barrier((up, down, before))
    blocks = (block, up, down, shifted(up[:middle], "y", 1), shifted(down[middle:], "y", -1))
    rows = jnp.concatenate([before, stream_in], axis=0).astype(F32)
    rows = rows * lax.rsqrt(jnp.mean(rows * rows, axis=1, keepdims=True) + epsilon) * norm_gain[0]
    rows = rows.astype(BF16)
    table = jnp.concatenate([conv_taps, channel_gain[:, None]], axis=1)
    small = in_parts(table).reshape(-1, cols)

    keep, send, later = call(
        functools.partial(first_kernel, cols, deep, lax.axis_size("y")),
        [
            ((half + HALO, cols), BF16),
            ((width + half + HALO + small.shape[0], cols), BF16),
            ((later.shape[0], 3 * cols), BF16),
        ],
        jnp.stack([y, c]),
        rows,
        small,
        *blocks,
        later,
        scratch=[((width, 2 * cols), BF16)],
        scalars=1,
    )
    later = lax.all_gather(
        later.reshape(-1, 1, deep, later.shape[1]), ("c", "y"), axis=1, tiled=True
    ).reshape(lax.axis_size("z"), 2, -1, later.shape[1])
    got = shifted(send, "c", 1)
    out_t = jnp.concatenate([send[:width], got[:width]], axis=1)
    padded, other_table = call(
        meet_kernel,
        [((half + HALO, 2 * cols), F32), ((2 * table.shape[1], cols), F32)],
        keep,
        got,
    )
    pair = (table, other_table.reshape(table.shape))
    ordered = jnp.where(c == 0, jnp.concatenate(pair, 2)[1], jnp.concatenate(pair[::-1], 2)[1])
    tables = (jnp.concatenate(pair, 2)[0], ordered)

    stream = lax.dynamic_slice_in_dim(stream_in, c * half, half, 0)
    for layer in range(2):
        if layer:
            gated, tail = call(
                functools.partial(second_kernel, cols),
                [((half, 2 * cols), BF16), ((HALO, 2 * cols), BF16)],
                stream,
                norm_gain[1:],
                later,
                scratch=[(stream.shape, BF16)],
                last=pl.BlockSpec((*later.shape[:3], 2 * cols), lambda _: (0, 0, 0, 0)),
            )
            columns, tail = lax.optimization_barrier((later, tail))
            columns = columns[..., 2 * cols :]
            out_t = jnp.concatenate([columns[:, k].reshape(width, cols) for k in range(2)], axis=1)
            padded = jnp.concatenate([passed_on(tail, (*SP, "c")), gated], axis=0).astype(F32)
        filtered = jnp.zeros((half, 2 * cols), F32)
        for tap in range(kernel):
            at = HALO - kernel + 1 + tap
            filtered = filtered + tables[layer][tap] * padded[at : at + half]
        sums = jnp.stack([jnp.sum(filtered, axis=1), jnp.sum(filtered * filtered, axis=1)])
        sums = jnp.sum(lax.all_gather(sums.reshape(1, -1), "x", axis=0), axis=0).reshape(2, half, 1)
        mean = sums[0] / width
        variance = sums[1] / width - mean * mean
        gain = tables[layer][kernel]
        activated = jax.nn.silu((filtered - mean) * lax.rsqrt(variance + epsilon) * gain).astype(BF16)
        branch = lax.dot_general(
            activated, out_t, (((1,), (1,)), ((), ())), preferred_element_type=F32
        ).astype(BF16)
        parts = lax.all_to_all(branch.reshape(xs, share, width), "x", 0, 0, tiled=True)
        own = lax.dynamic_slice_in_dim(stream, x * share, share, 0).astype(F32)
        own = (own + jnp.sum(parts.astype(F32), axis=0)).astype(BF16)
        stream = sent_to_all(own, "x").reshape(half, width)
    sibling = shifted(stream, "c", 1)
    return jnp.where(
        c == 0,
        jnp.concatenate([stream, sibling], axis=0),
        jnp.concatenate([sibling, stream], axis=0),
    )


def solution(mesh):
    finer = Mesh(mesh.devices.reshape(16, 4, 4, 2), (*SP, *TP))
    placed = (
        P(SP, None),
        P(),
        P(None, SP, TP),
        P(None, SP, TP),
        P(None, None, TP),
        P(None, TP),
        P(None, TP, SP),
    )
    return jax.shard_map(body, mesh=finer, in_specs=placed, out_specs=P(SP, None), check_vma=False)
```
